512 devices in a mesh: sp: 32 (over z, core), tp: 16 (over y, x).
Axes of the slice: x: 4, y: 4, z: 16, core: 2. Of those that a mesh axis runs over, the one named last changes fastest.
Arguments:
- tokens: bfloat16 [2, 24576, 4096], P(None, 'sp', 'tp'), may hold values from -6 to 6
- w_key: bfloat16 [4096, 2048], P(None, 'tp'), may hold values from -0.09375 to 0.09375
- w_value: bfloat16 [4096, 2048], P(None, 'tp'), may hold values from -0.09375 to 0.09375
- w_gate: bfloat16 [4096, 4, 16], replicated, may hold values from -0.09375 to 0.09375
- forget_bias: float32 [2, 16], replicated, may hold values from 3.9 to 13, as said below
- log_shift: float32 [2, 4, 16, 24576], P(None, None, 'tp', 'sp'), may hold values from -5 to 121, as said below
- new_query: bfloat16 [2, 4096, 2048], P(None, 'sp', 'tp'), may hold values from -6 to 6
Outputs:
- cache_matrix: bfloat16 [2, 2, 16, 128, 128], P(None, None, 'tp')
- cache_norm: float32 [2, 2, 16, 128], P(None, None, 'tp')
- cache_max: float32 [2, 2, 16], P(None, None, 'tp')
- first_read: bfloat16 [2, 4096, 2048], P(None, 'sp', 'tp')
The draws below stay inside these ranges and needn't reach their ends.
Inputs may be any that keep to these rules, and one draw needn't show every extreme that they name: `forget_bias`: added to the forget gates' pre-activations, by direction and head. `log_shift`: rows 0 and 2 are added to the input gates of the two directions; rows 1 and 3 are added to the log forget gates and are never positive.
All inputs are finite; a program needn't handle non-finite values.
Results may differ from the reference program's by a relative error of at most 0.024.
Values may be sent and summed in bfloat16 or wider, within the bound.
No kernel may reach another device: no remote copies, remote signals or barrier semaphores. Data moves between devices by JAX's collectives and lax.ppermute only.
A program may use at most 64 MiB of HBM per device.

```python
import math
import jax
import jax.numpy as jnp
from jax import lax

D = 4096
HEADS = 16
HEAD = 128
SEQS = 2
SEG = 768
CONTEXT_SPAN = 24576
NEW = 4096


def draw_forget_bias(key, part):
    pick_key, fast_key, slow_key = jax.random.split(jax.random.fold_in(key, 7), 3)
    slow_share = 0.5
    is_slow = jax.random.uniform(pick_key, (2, HEADS)) < slow_share
    fast_value = jax.random.uniform(fast_key, (2, HEADS), minval=3.9, maxval=5.0)
    slow_value = math.log(CONTEXT_SPAN) + 2.0 + jax.random.uniform(slow_key, (2, HEADS), minval=0.0, maxval=0.5)
    return jnp.where(is_slow, slow_value, fast_value).astype(jnp.float32)


def draw_log_shift(key, part):
    parallel_texts = jax.random.split(jax.random.fold_in(key, 13), 6)
    array_dimensions = (SEQS, 4, HEADS, CONTEXT_SPAN)
    inputs = jnp.clip(jax.random.normal(parallel_texts[0], array_dimensions), -4.0, 4.0)
    shrink_factor = jnp.exp(jax.random.uniform(parallel_texts[3], (SEQS, 1, HEADS, CONTEXT_SPAN // SEG), minval=math.log(0.25), maxval=0.0))
    shrink_factor = jnp.repeat(shrink_factor, SEG, axis=3)
    span_of_batch = jax.random.uniform(parallel_texts[4], array_dimensions) < 2.0 / CONTEXT_SPAN
    layer_stack_count = jax.random.uniform(parallel_texts[5], array_dimensions, minval=0.22, maxval=0.69)
    retention_switch = -shrink_factor / CONTEXT_SPAN - jnp.where(span_of_batch, layer_stack_count, 0.0)
    is_forget = (jnp.arange(4) % 2 == 1)[None, :, None, None]
    return jnp.where(is_forget, retention_switch, inputs).astype(jnp.float32)


def shard_levels(key, dims, cuts, least, top_value):
    gain, own = 1.0, jax.random.fold_in(key, 6)
    for dim, shards_of in cuts:
        steps = jnp.exp(jax.random.uniform(jax.random.fold_in(own, dim), (shards_of,), jnp.float32, least / len(cuts), top_value / len(cuts)))
        gain = gain * jnp.repeat(steps, dims[dim] // shards_of).reshape([-1 if axis == dim else 1 for axis in range(len(dims))])
    return gain


def scatter_about(rng, shape, spread, reach, cuts=(), kind=jnp.bfloat16):
    values = spread * jax.random.normal(rng, shape, jnp.float32)
    if cuts:
        values = values * shard_levels(rng, shape, cuts, -0.22, 0.18)
    return jnp.clip(values, -reach, reach).astype(kind)


def setup_inputs(seed: int = 0) -> dict:
    arg_keys = jax.random.split(jax.random.key(seed), 8)
    return {
        "tokens": scatter_about(arg_keys[0], (SEQS, CONTEXT_SPAN, D), 1.0, 6.0, ((1, 32), (2, 16))),
        "w_key": scatter_about(arg_keys[1], (D, HEADS * HEAD), D ** -0.5, 0.09375, ((1, 16),)),
        "w_value": scatter_about(arg_keys[2], (D, HEADS * HEAD), D ** -0.5, 0.09375, ((1, 16),)),
        "w_gate": scatter_about(arg_keys[3], (D, 4, HEADS), D ** -0.5, 0.09375),
        "forget_bias": draw_forget_bias(jax.random.fold_in(arg_keys[7], 71), 0),
        "log_shift": draw_log_shift(jax.random.fold_in(arg_keys[7], 71), 0),
        "new_query": scatter_about(arg_keys[6], (SEQS, NEW, HEADS * HEAD), 1.0, 6.0, ((1, 32), (2, 16))),
    }


def reference(tokens, w_key, w_value, w_gate, forget_bias, log_shift, new_query):
    flat_tokens = tokens.reshape(SEQS * CONTEXT_SPAN, D)
    key_rows = jnp.dot(flat_tokens, w_key, preferred_element_type=jnp.float32).astype(jnp.bfloat16)
    key_rows = key_rows.reshape(SEQS, CONTEXT_SPAN, HEADS, HEAD)
    value_rows = jnp.dot(flat_tokens, w_value, preferred_element_type=jnp.float32).astype(jnp.bfloat16)
    value_rows = value_rows.reshape(SEQS, CONTEXT_SPAN, HEADS, HEAD)
    gate_rows = jnp.dot(flat_tokens, w_gate.reshape(D, 4 * HEADS), preferred_element_type=jnp.float32)
    gate_rows = gate_rows.reshape(SEQS, CONTEXT_SPAN, 4, HEADS).transpose(0, 2, 3, 1)
    input_fwd = gate_rows[:, 0] + log_shift[:, 0]
    forget_fwd = jax.nn.log_sigmoid(gate_rows[:, 1] + forget_bias[0][None, :, None]) + log_shift[:, 1]
    input_bwd = gate_rows[:, 2] + log_shift[:, 2]
    forget_bwd = jax.nn.log_sigmoid(gate_rows[:, 3] + forget_bias[1][None, :, None]) + log_shift[:, 3]
    climb_fwd = jnp.cumsum(forget_fwd, axis=-1)
    total_fwd = climb_fwd[..., -1]
    weight_fwd = total_fwd[..., None] - climb_fwd + input_fwd
    climb_bwd = jnp.cumsum(forget_bwd, axis=-1)
    total_bwd = climb_bwd[..., -1]
    weight_bwd = climb_bwd - forget_bwd + input_bwd
    weights = jnp.stack([weight_fwd, weight_bwd], axis=1)
    totals = jnp.stack([total_fwd, total_bwd], axis=1)
    cache_max = jnp.maximum(totals, jnp.max(weights, axis=-1))
    scale_now = jnp.exp(weights - cache_max[..., None])
    key_f = key_rows.astype(jnp.float32).transpose(0, 2, 1, 3) * (HEAD ** -0.5)
    value_f = value_rows.astype(jnp.float32).transpose(0, 2, 1, 3)
    cache_norm = jnp.einsum('bjhl,bhld->bjhd', scale_now, key_f, precision=lax.Precision.HIGHEST)
    matrices = []
    for direction in range(2):
        weighted = scale_now[:, direction, :, :, None] * key_f
        matrices.append(jnp.einsum('bhld,bhle->bhde', weighted, value_f, precision=lax.Precision.HIGHEST))
    cache_matrix = jnp.stack(matrices, axis=1).astype(jnp.bfloat16)
    queries = new_query.reshape(SEQS, NEW, HEADS, HEAD).astype(jnp.float32)
    numerator = jnp.einsum('bthd,bjhde->bjthe', queries, cache_matrix.astype(jnp.float32))
    denominator = jnp.einsum('bthd,bjhd->bjth', queries, cache_norm, precision=lax.Precision.HIGHEST)
    divisor = jnp.maximum(jnp.abs(denominator), 1.0)
    first_read = jnp.sum(numerator / divisor[..., None], axis=1)
    first_read = first_read.reshape(SEQS, NEW, HEADS * HEAD).astype(jnp.bfloat16)
    return cache_matrix, cache_norm, cache_max, first_read
```

```python
import jax
import jax.numpy as jnp
from jax import lax
from jax.experimental import pallas as pl
from jax.experimental.pallas import tpu as pltpu
from jax.sharding import Mesh
from jax.sharding import PartitionSpec as P

HEAD = 128
SP = ("za", "zb", "c")
GROUP = ("zb", "c")
F32 = jnp.float32
BF16 = jnp.bfloat16


def shifted(array, core_axis, k):
    pairs = []
    for c in range(2):
        for y in range(4):
            for x in range(4):
                along_x = c == core_axis
                to = (y, (x + k) % 4) if along_x else ((y + k) % 4, x)
                pairs.append((c * 16 + y * 4 + x, c * 16 + to[0] * 4 + to[1]))
    return lax.ppermute(array, ("c", "y", "x"), pairs)


def gather_from(array, k):
    return shifted(array, 0, k)


def scatter_to(array, k):
    return shifted(array, 1, k)


def where_am_i():
    return lax.axis_index("c"), lax.axis_index("y"), lax.axis_index("x")


def feature_block(c, y, x, k, j):
    return jnp.where(c == 0, ((y + k) % 4) * 4 + (x - j + 4) % 4, ((y - j + 4) % 4) * 4 + (x + k) % 4)


def scatter_head(c, y, x, k):
    return jnp.where(c == 0, ((y + k) % 4) * 4 + x, y * 4 + (x + k) % 4)


def exchange(array, axes):
    return lax.all_to_all(array, axes, 0, 0, tiled=True)


def call(kernel, out_shape, flops=1000000, **more):
    return pl.pallas_call(
        kernel,
        out_shape=out_shape,
        cost_estimate=pl.CostEstimate(flops=flops, bytes_accessed=1000000, transcendentals=0),
        compiler_params=pltpu.CompilerParams(vmem_limit_bytes=48 * 1024 * 1024),
        **more,
    )


def shape(*dims, dtype=BF16):
    return jax.ShapeDtypeStruct(dims, dtype)


def pack_weights_kernel(wk_ref, wv_ref, *out_refs):
    c, y, x = where_am_i()
    part = out_refs[0].shape[0] // 4
    for k, out in enumerate(out_refs):
        for j in range(4):
            rows = pl.ds(feature_block(c, y, x, k, j) * part, part)
            out[j * part : (j + 1) * part, 0:128] = wk_ref[rows, :]
            out[j * part : (j + 1) * part, 128:256] = wv_ref[rows, :]


def pair_rows(values):
    row = lax.broadcasted_iota(jnp.int32, values.shape, 0)
    high = values.astype(BF16).astype(F32)
    return jnp.where(row < 4, high, values - high)


def store_gates(ref, p, top, values):
    paired = pair_rows(values)
    blocks = [paired[:, 256 * b : 256 * b + 256] for b in range(paired.shape[1] // 256)]
    blocks.append(jnp.zeros_like(blocks[0]))
    ref[p, top : top + 32, :] = jnp.concatenate(blocks, axis=0).astype(BF16)


def load_gates(tile):
    wide = tile.astype(F32)
    paired = jnp.concatenate([wide[8 * b : 8 * b + 8] for b in range(3)], axis=1)
    return paired + pltpu.roll(paired, 4, 0)


def project_kernel(t0_ref, t1_ref, t2_ref, t3_ref, w0_ref, w1_ref, w2_ref, w3_ref, gate_ref, o0, o1, o2, o3, g_ref):
    c, y, x = where_am_i()
    rows = t0_ref.shape[1]
    for p in range(t0_ref.shape[0]):
        piece = jnp.concatenate([t[p] for t in (t0_ref, t1_ref, t2_ref, t3_ref)], axis=1)
        weight = jnp.concatenate([gate_ref[feature_block(c, y, x, 0, j)] for j in range(4)], axis=1)
        g_ref[...] = lax.dot_general(weight, piece, (((1,), (1,)), ((), ())), preferred_element_type=F32)
        for k, (w_ref, out_ref) in enumerate(((w0_ref, o0), (w1_ref, o1), (w2_ref, o2), (w3_ref, o3))):
            total = jnp.dot(piece, w_ref[...], preferred_element_type=F32)
            out_ref[p, 0:rows, :] = total.astype(BF16)
            store_gates(out_ref, p, rows, g_ref[pl.ds(scatter_head(c, y, x, k) * 8, 8), :])


def log_sigmoid(v):
    return jnp.minimum(v, 0.0) - jnp.log1p(jnp.exp(-jnp.abs(v)))


def local_state(head, prompt, bias_ref, shift_ref, pieces):
    rows = shift_ref.shape[3]
    total = sum(ref[prompt, 0:rows, :].astype(F32) for ref in pieces)
    gates = sum(load_gates(ref[prompt, rows : rows + 32, :]) for ref in pieces)
    keys = total[:, 0:128].astype(BF16)
    values = total[:, 128:256].astype(BF16)
    length = gates.shape[1]
    shift = shift_ref[prompt, :, 0, :]
    row4 = lax.broadcasted_iota(jnp.int32, (4, length), 0)
    bias = jnp.where(row4 == 1, bias_ref[0, head], bias_ref[1, head])
    gates = gates[0:4, :]
    entry = gates + shift
    forget = log_sigmoid(gates + bias) + shift
    blocks = length // 128
    tall = jnp.concatenate([forget[:, 128 * b : 128 * b + 128] for b in range(blocks)], axis=0)
    r = lax.broadcasted_iota(jnp.int32, (128, 128), 0)
    c = lax.broadcasted_iota(jnp.int32, (128, 128), 1)
    climb = jnp.dot(tall, (r <= c).astype(F32), precision=lax.Precision.HIGHEST, preferred_element_type=F32)
    carry = jnp.zeros((4, 1), F32)
    parts = []
    for b in range(blocks):
        block = climb[4 * b : 4 * b + 4, :]
        parts.append(block + carry)
        carry = carry + block[:, 127:128]
    climb = jnp.concatenate(parts, axis=1)
    weight_fwd = carry[1:2] - climb[1:2] + entry[0:1]
    weight_bwd = climb[3:4] - forget[3:4] + entry[2:3]
    keys_t = jnp.transpose(keys.astype(F32))
    scale = HEAD ** -0.5
    memories, norms, tops, totals = [], [], [], []
    for weight, total in ((weight_fwd, carry[1:2]), (weight_bwd, carry[3:4])):
        top = jnp.max(weight, axis=1, keepdims=True)
        now = jnp.exp(weight - top)
        weighted = (keys_t * now).astype(BF16)
        memories.append(jnp.dot(weighted, values, preferred_element_type=F32) * scale)
        high = now.astype(BF16)
        low = (now - high.astype(F32)).astype(BF16)
        both = jnp.concatenate([high, low, jnp.zeros((6, length), BF16)], axis=0)
        norm = jnp.dot(both, keys, preferred_element_type=F32)
        norms.append((norm[0:1] + norm[1:2]) * scale)
        tops.append(jnp.broadcast_to(top, (1, 128)))
        totals.append(jnp.broadcast_to(total, (1, 128)))
    return memories, norms, totals, tops


def split_three(values):
    high = values.astype(BF16).astype(F32)
    rest = values - high
    middle = rest.astype(BF16).astype(F32)
    return high, middle, rest - middle


def small_tile(norms, totals, tops):
    norm_high = norms.astype(BF16).astype(F32)
    parts = split_three(jnp.concatenate([totals, tops], axis=0))
    return jnp.concatenate([norm_high, norms - norm_high, *parts], axis=0).astype(BF16)


def state_kernel(bias_ref, shift_ref, a_ref, b_ref, c_ref, d_ref, out_ref):
    head = lax.axis_index("y") * 4 + lax.axis_index("x")
    memories, norms, totals, tops = [], [], [], []
    for p in range(2):
        found = local_state(head, p, bias_ref, shift_ref, (a_ref, b_ref, c_ref, d_ref))
        for have, more in zip((memories, norms, totals, tops), found):
            have.extend(more)
    tile = small_tile(*(jnp.concatenate(v, axis=0) for v in (norms, totals, tops)))
    for g in range(8):
        for i in range(4):
            out_ref[g, 16 * i : 16 * i + 16, :] = memories[i][16 * g : 16 * g + 16, :].astype(BF16)
        out_ref[g, 64:96, :] = tile


def merged(in_ref, count):
    tiles = [in_ref[g, 64:96, :].astype(F32) for g in range(count)]
    norms = [t[0:4] + t[4:8] for t in tiles]
    scalars = [t[8:16] + t[16:24] + t[24:32] for t in tiles]
    totals = [s[0:4] for s in scalars]
    tops = [s[4:8] for s in scalars]
    row = lax.broadcasted_iota(jnp.int32, (4, 128), 0)
    before, after = [jnp.zeros((4, 128), F32)], [jnp.zeros((4, 128), F32)]
    for g in range(count - 1):
        before.append(before[-1] + totals[g])
        after.append(after[-1] + totals[count - 1 - g])
    whole = before[-1] + totals[-1]
    after = after[::-1]
    tops = [t + jnp.where(row % 2 == 0, after[g], before[g]) for g, t in enumerate(tops)]
    top = tops[0]
    for t in tops[1:]:
        top = jnp.maximum(top, t)
    return norms, tops, whole, top


def weighted_sums(in_ref, count, norms, tops, top):
    factors = [jnp.exp(t - top) for t in tops]
    norm = sum(f * n for f, n in zip(factors, norms))
    blocks = []
    for i in range(4):
        total = jnp.zeros((16, 128), F32)
        for g in range(count):
            total = total + in_ref[g, 16 * i : 16 * i + 16, :].astype(F32) * factors[g][i : i + 1]
        blocks.append(total)
    return norm, blocks


def group_merge_kernel(in_ref, out_ref):
    norms, tops, whole, top = merged(in_ref, 8)
    norm, blocks = weighted_sums(in_ref, 8, norms, tops, top)
    tile = small_tile(norm, whole, top)
    for g in range(4):
        for i in range(4):
            out_ref[g, 16 * i : 16 * i + 16, :] = blocks[i].astype(BF16)
        out_ref[g, 64:96, :] = tile


def last_merge_kernel(in_ref, out_ref, norm_ref, max_ref):
    norms, tops, whole, top = merged(in_ref, 4)
    top = jnp.maximum(whole, top)
    norm, blocks = weighted_sums(in_ref, 4, norms, tops, top)
    for g in range(8):
        for i in range(4):
            out_ref[g, 16 * i : 16 * i + 16, :] = blocks[i].astype(BF16)
    norm_ref[...] = norm
    max_ref[...] = top


def read_kernel(in_ref, norm_ref, query_ref, matrix_ref, read_ref):
    for g in range(8):
        for i in range(4):
            matrix_ref[i // 2, i % 2, 0, 16 * g : 16 * g + 16, :] = in_ref[g, 16 * i : 16 * i + 16, :]
    for p in range(2):
        query = query_ref[p]
        wide = query.astype(F32)
        total = jnp.zeros(wide.shape, F32)
        for j in range(2):
            i = 2 * p + j
            numerator = jnp.dot(query, matrix_ref[p, j, 0], preferred_element_type=F32)
            inner = jnp.sum(wide * norm_ref[i : i + 1, :], axis=1, keepdims=True)
            total = total + numerator / jnp.maximum(jnp.abs(inner), 1.0)
        read_ref[p] = total.astype(BF16)


def on_device(tokens, w_key, w_value, w_gate, forget_bias, log_shift, new_query):
    prompts, length, width = tokens.shape
    depth = 4 * width
    pieces = [tokens] + [gather_from(tokens, k) for k in (1, 2, 3)]
    weights = call(pack_weights_kernel, (shape(depth, 2 * HEAD),) * 4)(w_key, w_value)
    weights = [weights[0]] + [scatter_to(weights[k], k) for k in (1, 2, 3)]
    weights = [weights[0], weights[3], weights[2], weights[1]]
    gate = w_gate.transpose(2, 1, 0)
    gate = jnp.concatenate([gate, gate], axis=1).reshape(128, 16, width).transpose(1, 0, 2)
    out = shape(prompts, length + 32, 2 * HEAD)
    partial = call(
        project_kernel,
        (out,) * 4,
        flops=2 * prompts * length * depth * 1100,
        scratch_shapes=[pltpu.VMEM((128, length), F32)],
    )(*pieces, *weights, gate)
    partial = [partial[0]] + [scatter_to(partial[k], k) for k in (1, 2, 3)]
    smem = pl.BlockSpec(memory_space=pltpu.SMEM)
    vmem = pl.BlockSpec(memory_space=pltpu.VMEM)
    packed = call(state_kernel, shape(8, 96, HEAD), in_specs=[smem] + [vmem] * 5)(forget_bias, log_shift, *partial)
    grouped = call(group_merge_kernel, shape(4, 96, HEAD))(exchange(packed, GROUP))
    slices, norm, top = call(
        last_merge_kernel, (shape(8, 64, HEAD), shape(4, HEAD, dtype=F32), shape(4, HEAD, dtype=F32))
    )(exchange(grouped, "za"))
    matrix, read = call(read_kernel, (shape(2, 2, 1, HEAD, HEAD), shape(*new_query.shape)))(
        exchange(slices, GROUP), norm, new_query
    )
    return matrix, norm.reshape(2, 2, 1, HEAD), top[:, 0].reshape(2, 2, 1), read


def solution(mesh):
    finer = Mesh(mesh.devices.reshape(4, 4, 2, 4, 4), ("za", "zb", "c", "y", "x"))
    tp = ("y", "x")
    in_specs = (
        P(None, SP, tp),
        P(None, tp),
        P(None, tp),
        P(),
        P(),
        P(None, None, tp, SP),
        P(None, SP, tp),
    )
    out_specs = (
        P(None, None, tp, None, None),
        P(None, None, tp, None),
        P(None, None, tp),
        P(None, SP, tp),
    )
    return jax.shard_map(on_device, mesh=finer, in_specs=in_specs, out_specs=out_specs, check_vma=False)
```

```python
import functools

import jax
import jax.numpy as jnp
from jax import lax
from jax.experimental import pallas as pl
from jax.experimental.pallas import tpu as pltpu
from jax.sharding import Mesh
from jax.sharding import PartitionSpec as P


HEAD = 128
SP = ("za", "zb", "c")
GROUP = ("zb", "c")
F32 = jnp.float32
BF16 = jnp.bfloat16


def shifted(array, core_axis, k):
    pairs = []
    for c in range(2):
        for y in range(4):
            for x in range(4):
                along_x = c == core_axis
                to = (y, (x + k) % 4) if along_x else ((y + k) % 4, x)
                pairs.append((c * 16 + y * 4 + x, c * 16 + to[0] * 4 + to[1]))
    return lax.ppermute(array, ("c", "y", "x"), pairs)


def gather_from(array, k):
    return shifted(array, 0, k)


def scatter_to(array, k):
    return shifted(array, 1, k)


def where_am_i():
    return lax.axis_index("c"), lax.axis_index("y"), lax.axis_index("x")


def feature_block(c, y, x, k, j):
    return jnp.where(c == 0, ((y + k) % 4) * 4 + (x - j + 4) % 4, ((y - j + 4) % 4) * 4 + (x + k) % 4)


def scatter_head(c, y, x, k):
    return jnp.where(c == 0, ((y + k) % 4) * 4 + x, y * 4 + (x + k) % 4)


def exchange(array, axes):
    return lax.all_to_all(array, axes, 0, 0, tiled=True)


def call(kernel, out_shape, flops=1000000, **more):
    return pl.pallas_call(
        kernel,
        out_shape=out_shape,
        cost_estimate=pl.CostEstimate(flops=flops, bytes_accessed=1000000, transcendentals=0),
        compiler_params=pltpu.CompilerParams(vmem_limit_bytes=48 * 1024 * 1024),
        **more,
    )


def shape(*dims, dtype=BF16):
    return jax.ShapeDtypeStruct(dims, dtype)


def pack_weights_kernel(wk_ref, wv_ref, *out_refs):
    c, y, x = where_am_i()
    part = out_refs[0].shape[0] // 4
    for k, out in enumerate(out_refs):
        for j in range(4):
            rows = pl.ds(feature_block(c, y, x, k, j) * part, part)
            out[j * part : (j + 1) * part, 0:128] = wk_ref[rows, :]
            out[j * part : (j + 1) * part, 128:256] = wv_ref[rows, :]


def pair_rows(values):
    row = lax.broadcasted_iota(jnp.int32, values.shape, 0)
    high = values.astype(BF16).astype(F32)
    return jnp.where(row < 4, high, values - high)


def store_gates(ref, p, top, values):
    paired = pair_rows(values)
    blocks = [paired[:, 256 * b : 256 * b + 256] for b in range(paired.shape[1] // 256)]
    blocks.append(jnp.zeros_like(blocks[0]))
    ref[p, top : top + 32, :] = jnp.concatenate(blocks, axis=0).astype(BF16)


def load_gates(tile):
    wide = tile.astype(F32)
    paired = jnp.concatenate([wide[8 * b : 8 * b + 8] for b in range(3)], axis=1)
    return paired + pltpu.roll(paired, 4, 0)


def gates_kernel(t0_ref, t1_ref, t2_ref, t3_ref, gate_ref, out_ref):
    c, y, x = where_am_i()
    weight = jnp.concatenate([gate_ref[feature_block(c, y, x, 0, j)] for j in range(4)], axis=1)
    for p in range(t0_ref.shape[0]):
        piece = jnp.concatenate([t[p] for t in (t0_ref, t1_ref, t2_ref, t3_ref)], axis=1)
        out_ref[p] = lax.dot_general(weight, piece, (((1,), (1,)), ((), ())), preferred_element_type=F32)


def project_kernel(k, t0_ref, t1_ref, t2_ref, t3_ref, w_ref, gates_ref, out_ref):
    c, y, x = where_am_i()
    rows = t0_ref.shape[1]
    for p in range(t0_ref.shape[0]):
        piece = jnp.concatenate([t[p] for t in (t0_ref, t1_ref, t2_ref, t3_ref)], axis=1)
        total = jnp.dot(piece, w_ref[...], preferred_element_type=F32)
        out_ref[p, 0:rows, :] = total.astype(BF16)
        store_gates(out_ref, p, rows, gates_ref[p, pl.ds(scatter_head(c, y, x, k) * 8, 8), :])


def log_sigmoid(v):
    return jnp.minimum(v, 0.0) - jnp.log1p(jnp.exp(-jnp.abs(v)))


def local_state(head, prompt, bias_ref, shift_ref, pieces):
    rows = shift_ref.shape[3]
    total = sum(ref[prompt, 0:rows, :].astype(F32) for ref in pieces)
    gates = sum(load_gates(ref[prompt, rows : rows + 32, :]) for ref in pieces)
    keys = total[:, 0:128].astype(BF16)
    values = total[:, 128:256].astype(BF16)
    length = gates.shape[1]
    shift = shift_ref[prompt, :, 0, :]
    row4 = lax.broadcasted_iota(jnp.int32, (4, length), 0)
    bias = jnp.where(row4 == 1, bias_ref[0, head], bias_ref[1, head])
    gates = gates[0:4, :]
    entry = gates + shift
    forget = log_sigmoid(gates + bias) + shift
    blocks = length // 128
    tall = jnp.concatenate([forget[:, 128 * b : 128 * b + 128] for b in range(blocks)], axis=0)
    r = lax.broadcasted_iota(jnp.int32, (128, 128), 0)
    c = lax.broadcasted_iota(jnp.int32, (128, 128), 1)
    climb = jnp.dot(tall, (r <= c).astype(F32), precision=lax.Precision.HIGHEST, preferred_element_type=F32)
    carry = jnp.zeros((4, 1), F32)
    parts = []
    for b in range(blocks):
        block = climb[4 * b : 4 * b + 4, :]
        parts.append(block + carry)
        carry = carry + block[:, 127:128]
    climb = jnp.concatenate(parts, axis=1)
    weight_fwd = carry[1:2] - climb[1:2] + entry[0:1]
    weight_bwd = climb[3:4] - forget[3:4] + entry[2:3]
    keys_t = jnp.transpose(keys.astype(F32))
    scale = HEAD ** -0.5
    memories, norms, tops, totals = [], [], [], []
    for weight, total in ((weight_fwd, carry[1:2]), (weight_bwd, carry[3:4])):
        top = jnp.max(weight, axis=1, keepdims=True)
        now = jnp.exp(weight - top)
        weighted = (keys_t * now).astype(BF16)
        memories.append(jnp.dot(weighted, values, preferred_element_type=F32) * scale)
        high = now.astype(BF16)
        low = (now - high.astype(F32)).astype(BF16)
        both = jnp.concatenate([high, low, jnp.zeros((6, length), BF16)], axis=0)
        norm = jnp.dot(both, keys, preferred_element_type=F32)
        norms.append((norm[0:1] + norm[1:2]) * scale)
        tops.append(jnp.broadcast_to(top, (1, 128)))
        totals.append(jnp.broadcast_to(total, (1, 128)))
    return memories, norms, totals, tops


def split_three(values):
    high = values.astype(BF16).astype(F32)
    rest = values - high
    middle = rest.astype(BF16).astype(F32)
    return high, middle, rest - middle


def small_tile(norms, totals, tops):
    norm_high = norms.astype(BF16).astype(F32)
    parts = split_three(jnp.concatenate([totals, tops], axis=0))
    return jnp.concatenate([norm_high, norms - norm_high, *parts], axis=0).astype(BF16)


def state_kernel(bias_ref, shift_ref, a_ref, b_ref, c_ref, d_ref, out_ref):
    head = lax.axis_index("y") * 4 + lax.axis_index("x")
    memories, norms, totals, tops = [], [], [], []
    for p in range(2):
        found = local_state(head, p, bias_ref, shift_ref, (a_ref, b_ref, c_ref, d_ref))
        for have, more in zip((memories, norms, totals, tops), found):
            have.extend(more)
    tile = small_tile(*(jnp.concatenate(v, axis=0) for v in (norms, totals, tops)))
    for g in range(8):
        for i in range(4):
            out_ref[g, 16 * i : 16 * i + 16, :] = memories[i][16 * g : 16 * g + 16, :].astype(BF16)
        out_ref[g, 64:96, :] = tile


def merged(in_ref, count):
    tiles = [in_ref[g, 64:96, :].astype(F32) for g in range(count)]
    norms = [t[0:4] + t[4:8] for t in tiles]
    scalars = [t[8:16] + t[16:24] + t[24:32] for t in tiles]
    totals = [s[0:4] for s in scalars]
    tops = [s[4:8] for s in scalars]
    row = lax.broadcasted_iota(jnp.int32, (4, 128), 0)
    before, after = [jnp.zeros((4, 128), F32)], [jnp.zeros((4, 128), F32)]
    for g in range(count - 1):
        before.append(before[-1] + totals[g])
        after.append(after[-1] + totals[count - 1 - g])
    whole = before[-1] + totals[-1]
    after = after[::-1]
    tops = [t + jnp.where(row % 2 == 0, after[g], before[g]) for g, t in enumerate(tops)]
    top = tops[0]
    for t in tops[1:]:
        top = jnp.maximum(top, t)
    return norms, tops, whole, top


def weighted_sums(in_ref, count, norms, tops, top):
    factors = [jnp.exp(t - top) for t in tops]
    norm = sum(f * n for f, n in zip(factors, norms))
    blocks = []
    for i in range(4):
        total = jnp.zeros((16, 128), F32)
        for g in range(count):
            total = total + in_ref[g, 16 * i : 16 * i + 16, :].astype(F32) * factors[g][i : i + 1]
        blocks.append(total)
    return norm, blocks


def group_merge_kernel(in_ref, out_ref):
    norms, tops, whole, top = merged(in_ref, 8)
    norm, blocks = weighted_sums(in_ref, 8, norms, tops, top)
    tile = small_tile(norm, whole, top)
    for g in range(4):
        for i in range(4):
            out_ref[g, 16 * i : 16 * i + 16, :] = blocks[i].astype(BF16)
        out_ref[g, 64:96, :] = tile


def last_merge_kernel(in_ref, out_ref, norm_ref, max_ref):
    norms, tops, whole, top = merged(in_ref, 4)
    top = jnp.maximum(whole, top)
    norm, blocks = weighted_sums(in_ref, 4, norms, tops, top)
    for g in range(8):
        for i in range(4):
            out_ref[g, 16 * i : 16 * i + 16, :] = blocks[i].astype(BF16)
    norm_ref[...] = norm
    max_ref[...] = top


def read_kernel(in_ref, norm_ref, query_ref, matrix_ref, read_ref):
    for g in range(8):
        for i in range(4):
            matrix_ref[i // 2, i % 2, 0, 16 * g : 16 * g + 16, :] = in_ref[g, 16 * i : 16 * i + 16, :]
    for p in range(2):
        query = query_ref[p]
        wide = query.astype(F32)
        total = jnp.zeros(wide.shape, F32)
        for j in range(2):
            i = 2 * p + j
            numerator = jnp.dot(query, matrix_ref[p, j, 0], preferred_element_type=F32)
            inner = jnp.sum(wide * norm_ref[i : i + 1, :], axis=1, keepdims=True)
            total = total + numerator / jnp.maximum(jnp.abs(inner), 1.0)
        read_ref[p] = total.astype(BF16)


def program(tokens, w_key, w_value, w_gate, forget_bias, log_shift, new_query):
    prompts, length, width = tokens.shape
    depth = 4 * width
    pieces = [tokens] + [gather_from(tokens, k) for k in (1, 2, 3)]
    weights = call(pack_weights_kernel, (shape(depth, 2 * HEAD),) * 4)(w_key, w_value)
    weights = [weights[0]] + [scatter_to(weights[k], k) for k in (1, 2, 3)]
    weights = [weights[0], weights[3], weights[2], weights[1]]
    gate = w_gate.transpose(2, 1, 0)
    gate = jnp.concatenate([gate, gate], axis=1).reshape(128, 16, width).transpose(1, 0, 2)
    gates = call(gates_kernel, shape(prompts, 128, length, dtype=F32))(*pieces, gate)
    partial = []
    for k in range(4):
        project = call(
            functools.partial(project_kernel, k),
            shape(prompts, length + 32, 2 * HEAD),
            flops=2 * prompts * length * depth * 256,
        )
        part = project(*pieces, weights[k], gates)
        partial.append(scatter_to(part, k) if k else part)
    smem = pl.BlockSpec(memory_space=pltpu.SMEM)
    vmem = pl.BlockSpec(memory_space=pltpu.VMEM)
    packed = call(state_kernel, shape(8, 96, HEAD), in_specs=[smem] + [vmem] * 5)(forget_bias, log_shift, *partial)
    grouped = call(group_merge_kernel, shape(4, 96, HEAD))(exchange(packed, GROUP))
    slices, norm, top = call(
        last_merge_kernel, (shape(8, 64, HEAD), shape(4, HEAD, dtype=F32), shape(4, HEAD, dtype=F32))
    )(exchange(grouped, "za"))
    matrix, read = call(read_kernel, (shape(2, 2, 1, HEAD, HEAD), shape(*new_query.shape)))(
        exchange(slices, GROUP), norm, new_query
    )
    return matrix, norm.reshape(2, 2, 1, HEAD), top[:, 0].reshape(2, 2, 1), read


def solution(mesh):
    finer = Mesh(mesh.devices.reshape(4, 4, 2, 4, 4), ("za", "zb", "c", "y", "x"))
    tp = ("y", "x")
    in_specs = (
        P(None, SP, tp),
        P(None, tp),
        P(None, tp),
        P(),
        P(),
        P(None, None, tp, SP),
        P(None, SP, tp),
    )
    out_specs = (
        P(None, None, tp, None, None),
        P(None, None, tp, None),
        P(None, None, tp),
        P(None, SP, tp),
    )
    return jax.shard_map(program, mesh=finer, in_specs=in_specs, out_specs=out_specs, check_vma=False)
```

```python
import functools

import jax
import jax.numpy as jnp
from jax import lax
from jax.experimental import pallas as pl
from jax.experimental.pallas import tpu as pltpu
from jax.sharding import Mesh
from jax.sharding import PartitionSpec as P


HEAD = 128
SP = ("za", "zb", "c")
GROUP = ("zb", "c")
F32 = jnp.float32
BF16 = jnp.bfloat16


def shifted(array, core_axis, k):
    pairs = []
    for c in range(2):
        for y in range(4):
            for x in range(4):
                along_x = c == core_axis
                to = (y, (x + k) % 4) if along_x else ((y + k) % 4, x)
                pairs.append((c * 16 + y * 4 + x, c * 16 + to[0] * 4 + to[1]))
    return lax.ppermute(array, ("c", "y", "x"), pairs)


def gather_from(array, k):
    return shifted(array, 0, k)


def scatter_to(array, k):
    return shifted(array, 1, k)


def where_am_i():
    return lax.axis_index("c"), lax.axis_index("y"), lax.axis_index("x")


def feature_block(c, y, x, k, j):
    return jnp.where(c == 0, ((y + k) % 4) * 4 + (x - j + 4) % 4, ((y - j + 4) % 4) * 4 + (x + k) % 4)


def scatter_head(c, y, x, k):
    return jnp.where(c == 0, ((y + k) % 4) * 4 + x, y * 4 + (x + k) % 4)


def exchange(array, axes):
    return lax.all_to_all(array, axes, 0, 0, tiled=True)


def call(kernel, out_shape, flops=1000000, **more):
    return pl.pallas_call(
        kernel,
        out_shape=out_shape,
        cost_estimate=pl.CostEstimate(flops=flops, bytes_accessed=1000000, transcendentals=0),
        compiler_params=pltpu.CompilerParams(vmem_limit_bytes=48 * 1024 * 1024),
        **more,
    )


def shape(*dims, dtype=BF16):
    return jax.ShapeDtypeStruct(dims, dtype)


def pack_weights_kernel(wk_ref, wv_ref, *out_refs):
    c, y, x = where_am_i()
    part = out_refs[0].shape[0] // 4
    for k, out in enumerate(out_refs):
        for j in range(4):
            rows = pl.ds(feature_block(c, y, x, k, j) * part, part)
            out[j * part : (j + 1) * part, 0:128] = wk_ref[rows, :]
            out[j * part : (j + 1) * part, 128:256] = wv_ref[rows, :]


def pair_rows(values):
    row = lax.broadcasted_iota(jnp.int32, values.shape, 0)
    high = values.astype(BF16).astype(F32)
    return jnp.where(row < 4, high, values - high)


def store_gates(ref, p, top, values):
    paired = pair_rows(values)
    blocks = [paired[:, 256 * b : 256 * b + 256] for b in range(paired.shape[1] // 256)]
    blocks.append(jnp.zeros_like(blocks[0]))
    ref[p, top : top + 32, :] = jnp.concatenate(blocks, axis=0).astype(BF16)


def load_gates(tile):
    wide = tile.astype(F32)
    paired = jnp.concatenate([wide[8 * b : 8 * b + 8] for b in range(3)], axis=1)
    return paired + pltpu.roll(paired, 4, 0)


def joined(p, t0_ref, t1_ref, far_a_ref, far_b_ref, t3_ref):
    far_ref = far_b_ref if p else far_a_ref
    return jnp.concatenate([t0_ref[p], t1_ref[p], far_ref[0], t3_ref[p]], axis=1)


def gates_kernel(*refs):
    *piece_refs, gate_ref, out_ref = refs
    c, y, x = where_am_i()
    weight = jnp.concatenate([gate_ref[feature_block(c, y, x, 0, j)] for j in range(4)], axis=1)
    for p in range(2):
        piece = joined(p, *piece_refs)
        out_ref[p] = lax.dot_general(weight, piece, (((1,), (1,)), ((), ())), preferred_element_type=F32)


def project_kernel(k, *refs):
    *piece_refs, w_ref, gates_ref, out_ref = refs
    c, y, x = where_am_i()
    rows = piece_refs[0].shape[1]
    for p in range(2):
        piece = joined(p, *piece_refs)
        total = jnp.dot(piece, w_ref[...], preferred_element_type=F32)
        out_ref[p, 0:rows, :] = total.astype(BF16)
        store_gates(out_ref, p, rows, gates_ref[p, pl.ds(scatter_head(c, y, x, k) * 8, 8), :])


def log_sigmoid(v):
    return jnp.minimum(v, 0.0) - jnp.log1p(jnp.exp(-jnp.abs(v)))


def local_state(head, prompt, bias_ref, shift_ref, pieces):
    rows = shift_ref.shape[3]
    total = sum(ref[prompt, 0:rows, :].astype(F32) for ref in pieces)
    gates = sum(load_gates(ref[prompt, rows : rows + 32, :]) for ref in pieces)
    keys = total[:, 0:128].astype(BF16)
    values = total[:, 128:256].astype(BF16)
    length = gates.shape[1]
    shift = shift_ref[prompt, :, 0, :]
    row4 = lax.broadcasted_iota(jnp.int32, (4, length), 0)
    bias = jnp.where(row4 == 1, bias_ref[0, head], bias_ref[1, head])
    gates = gates[0:4, :]
    entry = gates + shift
    forget = log_sigmoid(gates + bias) + shift
    blocks = length // 128
    tall = jnp.concatenate([forget[:, 128 * b : 128 * b + 128] for b in range(blocks)], axis=0)
    r = lax.broadcasted_iota(jnp.int32, (128, 128), 0)
    c = lax.broadcasted_iota(jnp.int32, (128, 128), 1)
    climb = jnp.dot(tall, (r <= c).astype(F32), precision=lax.Precision.HIGHEST, preferred_element_type=F32)
    carry = jnp.zeros((4, 1), F32)
    parts = []
    for b in range(blocks):
        block = climb[4 * b : 4 * b + 4, :]
        parts.append(block + carry)
        carry = carry + block[:, 127:128]
    climb = jnp.concatenate(parts, axis=1)
    weight_fwd = carry[1:2] - climb[1:2] + entry[0:1]
    weight_bwd = climb[3:4] - forget[3:4] + entry[2:3]
    keys_t = jnp.transpose(keys.astype(F32))
    scale = HEAD ** -0.5
    memories, norms, tops, totals = [], [], [], []
    for weight, total in ((weight_fwd, carry[1:2]), (weight_bwd, carry[3:4])):
        top = jnp.max(weight, axis=1, keepdims=True)
        now = jnp.exp(weight - top)
        weighted = (keys_t * now).astype(BF16)
        memories.append(jnp.dot(weighted, values, preferred_element_type=F32) * scale)
        high = now.astype(BF16)
        low = (now - high.astype(F32)).astype(BF16)
        both = jnp.concatenate([high, low, jnp.zeros((6, length), BF16)], axis=0)
        norm = jnp.dot(both, keys, preferred_element_type=F32)
        norms.append((norm[0:1] + norm[1:2]) * scale)
        tops.append(jnp.broadcast_to(top, (1, 128)))
        totals.append(jnp.broadcast_to(total, (1, 128)))
    return memories, norms, totals, tops


def split_three(values):
    high = values.astype(BF16).astype(F32)
    rest = values - high
    middle = rest.astype(BF16).astype(F32)
    return high, middle, rest - middle


def small_tile(norms, totals, tops):
    norm_high = norms.astype(BF16).astype(F32)
    high, middle, low = split_three(jnp.concatenate([totals, tops], axis=0))
    lane = lax.broadcasted_iota(jnp.int32, high.shape, 1)
    parts = jnp.where(lane < 32, high, jnp.where(lane < 64, middle, low))
    return jnp.concatenate([norm_high, norms - norm_high, parts], axis=0).astype(BF16)


def state_kernel(bias_ref, shift_ref, a_ref, b_ref, c_ref, d_ref, out_ref):
    head = lax.axis_index("y") * 4 + lax.axis_index("x")
    memories, norms, totals, tops = [], [], [], []
    for p in range(2):
        found = local_state(head, p, bias_ref, shift_ref, (a_ref, b_ref, c_ref, d_ref))
        for have, more in zip((memories, norms, totals, tops), found):
            have.extend(more)
    tile = small_tile(*(jnp.concatenate(v, axis=0) for v in (norms, totals, tops)))
    for g in range(8):
        for i in range(4):
            out_ref[g, 16 * i : 16 * i + 16, :] = memories[i][16 * g : 16 * g + 16, :].astype(BF16)
        out_ref[g, 64:80, :] = tile


def merged(in_ref, count):
    tiles = [in_ref[g, 64:80, :].astype(F32) for g in range(count)]
    norms = [t[0:4] + t[4:8] for t in tiles]
    scalars = []
    for t in tiles:
        parts = t[8:16]
        whole = parts[:, 0:1] + parts[:, 32:33] + parts[:, 64:65]
        scalars.append(jnp.broadcast_to(whole, (8, 128)))
    totals = [s[0:4] for s in scalars]
    tops = [s[4:8] for s in scalars]
    row = lax.broadcasted_iota(jnp.int32, (4, 128), 0)
    before, after = [jnp.zeros((4, 128), F32)], [jnp.zeros((4, 128), F32)]
    for g in range(count - 1):
        before.append(before[-1] + totals[g])
        after.append(after[-1] + totals[count - 1 - g])
    whole = before[-1] + totals[-1]
    after = after[::-1]
    tops = [t + jnp.where(row % 2 == 0, after[g], before[g]) for g, t in enumerate(tops)]
    top = tops[0]
    for t in tops[1:]:
        top = jnp.maximum(top, t)
    return norms, tops, whole, top


def weighted_sums(in_ref, count, norms, tops, top):
    factors = [jnp.exp(t - top) for t in tops]
    norm = sum(f * n for f, n in zip(factors, norms))
    blocks = []
    for i in range(4):
        total = jnp.zeros((16, 128), F32)
        for g in range(count):
            total = total + in_ref[g, 16 * i : 16 * i + 16, :].astype(F32) * factors[g][i : i + 1]
        blocks.append(total)
    return norm, blocks


def group_merge_kernel(in_ref, out_ref):
    norms, tops, whole, top = merged(in_ref, 8)
    norm, blocks = weighted_sums(in_ref, 8, norms, tops, top)
    tile = small_tile(norm, whole, top)
    for g in range(4):
        for i in range(4):
            out_ref[g, 16 * i : 16 * i + 16, :] = blocks[i].astype(BF16)
        out_ref[g, 64:80, :] = tile


def last_merge_kernel(in_ref, out_ref, norm_ref, max_ref):
    norms, tops, whole, top = merged(in_ref, 4)
    top = jnp.maximum(whole, top)
    norm, blocks = weighted_sums(in_ref, 4, norms, tops, top)
    for g in range(8):
        for i in range(4):
            out_ref[g, 16 * i : 16 * i + 16, :] = blocks[i].astype(BF16)
    for i in range(4):
        norm_ref[i // 2, i % 2, :, :] = norm[i : i + 1]
        max_ref[i // 2, i % 2 : i % 2 + 1, :] = top[i : i + 1, 0:1]


def read_kernel(in_ref, norm_ref, query_ref, matrix_ref, read_ref):
    for g in range(8):
        for i in range(4):
            matrix_ref[i // 2, i % 2, 0, 16 * g : 16 * g + 16, :] = in_ref[g, 16 * i : 16 * i + 16, :]
    for p in range(2):
        query = query_ref[p]
        wide = query.astype(F32)
        total = jnp.zeros(wide.shape, F32)
        for j in range(2):
            i = 2 * p + j
            numerator = jnp.dot(query, matrix_ref[p, j, 0], preferred_element_type=F32)
            inner = jnp.sum(wide * norm_ref[p, j, :, :], axis=1, keepdims=True)
            total = total + numerator / jnp.maximum(jnp.abs(inner), 1.0)
        read_ref[p] = total.astype(BF16)


def program(tokens, w_key, w_value, w_gate, forget_bias, log_shift, new_query):
    prompts, length, width = tokens.shape
    depth = 4 * width
    near = {k: gather_from(tokens, k) for k in (1, 3)}
    far = [gather_from(near[k][p : p + 1], k) for p, k in enumerate((1, 3))]
    pieces = [tokens, near[1], *far, near[3]]
    weights = call(pack_weights_kernel, (shape(depth, 2 * HEAD),) * 4)(w_key, w_value)
    weights = [weights[0]] + [scatter_to(weights[k], k) for k in (1, 2, 3)]
    weights = [weights[0], weights[3], weights[2], weights[1]]
    gate = w_gate.transpose(2, 1, 0)
    gate = jnp.concatenate([gate, gate], axis=1).reshape(128, 16, width).transpose(1, 0, 2)
    gates = call(gates_kernel, shape(prompts, 128, length, dtype=F32))(*pieces, gate)
    partial = []
    for k in range(4):
        project = call(
            functools.partial(project_kernel, k),
            shape(prompts, length + 32, 2 * HEAD),
            flops=2 * prompts * length * depth * 256,
        )
        part = project(*pieces, weights[k], gates)
        partial.append(scatter_to(part, k) if k else part)
    smem = pl.BlockSpec(memory_space=pltpu.SMEM)
    vmem = pl.BlockSpec(memory_space=pltpu.VMEM)
    packed = call(state_kernel, shape(8, 80, HEAD), in_specs=[smem] + [vmem] * 5)(forget_bias, log_shift, *partial)
    grouped = call(group_merge_kernel, shape(4, 80, HEAD))(exchange(packed, GROUP))
    slices, norm, top = call(
        last_merge_kernel, (shape(8, 64, HEAD), shape(2, 2, 1, HEAD, dtype=F32), shape(2, 2, 1, dtype=F32))
    )(exchange(grouped, "za"))
    matrix, read = call(read_kernel, (shape(2, 2, 1, HEAD, HEAD), shape(*new_query.shape)))(
        exchange(slices, GROUP), norm, new_query
    )
    return matrix, norm, top, read


def solution(mesh):
    finer = Mesh(mesh.devices.reshape(4, 4, 2, 4, 4), ("za", "zb", "c", "y", "x"))
    tp = ("y", "x")
    in_specs = (
        P(None, SP, tp),
        P(None, tp),
        P(None, tp),
        P(),
        P(),
        P(None, None, tp, SP),
        P(None, SP, tp),
    )
    out_specs = (
        P(None, None, tp, None, None),
        P(None, None, tp, None),
        P(None, None, tp),
        P(None, SP, tp),
    )
    return jax.shard_map(program, mesh=finer, in_specs=in_specs, out_specs=out_specs, check_vma=False)
```

```python
import functools

import jax
import jax.numpy as jnp
from jax import lax
from jax.experimental import pallas as pl
from jax.experimental.pallas import tpu as pltpu
from jax.sharding import Mesh
from jax.sharding import PartitionSpec as P


HEAD = 128
SP = ("za", "zb", "c")
GROUP = ("zb", "c")
F32 = jnp.float32
BF16 = jnp.bfloat16


def shifted(array, core_axis, k):
    pairs = []
    for c in range(2):
        for y in range(4):
            for x in range(4):
                along_x = c == core_axis
                to = (y, (x + k) % 4) if along_x else ((y + k) % 4, x)
                pairs.append((c * 16 + y * 4 + x, c * 16 + to[0] * 4 + to[1]))
    return lax.ppermute(array, ("c", "y", "x"), pairs)


def gather_from(array, k):
    return shifted(array, 0, k)


def scatter_to(array, k):
    return shifted(array, 1, k)


def where_am_i():
    return lax.axis_index("c"), lax.axis_index("y"), lax.axis_index("x")


def feature_block(c, y, x, k, j):
    return jnp.where(c == 0, ((y + k) % 4) * 4 + (x - j + 4) % 4, ((y - j + 4) % 4) * 4 + (x + k) % 4)


def scatter_head(c, y, x, k):
    return jnp.where(c == 0, ((y + k) % 4) * 4 + x, y * 4 + (x + k) % 4)


def exchange(array, axes):
    return lax.all_to_all(array, axes, 0, 0, tiled=True)


def call(kernel, out_shape, flops=1000000, **more):
    return pl.pallas_call(
        kernel,
        out_shape=out_shape,
        cost_estimate=pl.CostEstimate(flops=flops, bytes_accessed=1000000, transcendentals=0),
        compiler_params=pltpu.CompilerParams(vmem_limit_bytes=48 * 1024 * 1024),
        **more,
    )


def shape(*dims, dtype=BF16):
    return jax.ShapeDtypeStruct(dims, dtype)


def first_of_pair():
    return lax.axis_index("zb") % 2 == 0


def pack_weights_kernel(wk_ref, wv_ref, *out_refs):
    c, y, x = where_am_i()
    part = out_refs[0].shape[0] // 4
    for k, out in enumerate(out_refs):
        for j in range(4):
            rows = pl.ds(feature_block(c, y, x, k, j) * part, part)
            here = slice(j * part, (j + 1) * part)
            if k == 2:

                @pl.when(first_of_pair())
                def _(out=out, here=here, rows=rows):
                    out[here, :] = wk_ref[rows, :]

                @pl.when(jnp.logical_not(first_of_pair()))
                def _(out=out, here=here, rows=rows):
                    out[here, :] = wv_ref[rows, :]
            else:
                out[here, 0:128] = wk_ref[rows, :]
                out[here, 128:256] = wv_ref[rows, :]


def pair_rows(values):
    row = lax.broadcasted_iota(jnp.int32, values.shape, 0)
    high = values.astype(BF16).astype(F32)
    return jnp.where(row < 4, high, values - high)


def store_gates(ref, p, top, values):
    paired = pair_rows(values)
    blocks = [paired[:, 256 * b : 256 * b + 256] for b in range(paired.shape[1] // 256)]
    blocks.append(jnp.zeros_like(blocks[0]))
    ref[p, top : top + 32, :] = jnp.concatenate(blocks, axis=0).astype(BF16)


def load_gates(tile):
    wide = tile.astype(F32)
    paired = jnp.concatenate([wide[8 * b : 8 * b + 8] for b in range(3)], axis=1)
    return paired + pltpu.roll(paired, 4, 0)


def joined(p, t0_ref, t1_ref, far_a_ref, far_b_ref, t3_ref):
    far_ref = far_b_ref if p else far_a_ref
    return jnp.concatenate([t0_ref[p], t1_ref[p], far_ref[0], t3_ref[p]], axis=1)


def gates_kernel(*refs):
    *piece_refs, gate_ref, out_ref = refs
    c, y, x = where_am_i()
    weight = jnp.concatenate([gate_ref[feature_block(c, y, x, 0, j)] for j in range(4)], axis=1)
    for p in range(2):
        piece = joined(p, *piece_refs)
        out_ref[p] = lax.dot_general(weight, piece, (((1,), (1,)), ((), ())), preferred_element_type=F32)


def project_kernel(k, *refs):
    *in_refs, gates_ref, out_ref = refs
    piece_refs, w_refs = in_refs[:5], in_refs[5:]
    c, y, x = where_am_i()
    rows = piece_refs[0].shape[1]
    weight = jnp.concatenate([w[...] for w in w_refs], axis=1)
    for p in range(2):
        piece = joined(p, *piece_refs)
        total = jnp.dot(piece, weight, preferred_element_type=F32)
        if len(w_refs) == 2:
            own, other = total[:, 0:128], total[:, 128:256]
            first = first_of_pair()
            total = jnp.concatenate([jnp.where(first, own, other), jnp.where(first, other, own)], axis=1)
        out_ref[p, 0:rows, :] = total.astype(BF16)
        store_gates(out_ref, p, rows, gates_ref[p, pl.ds(scatter_head(c, y, x, k) * 8, 8), :])


def log_sigmoid(v):
    return jnp.minimum(v, 0.0) - jnp.log1p(jnp.exp(-jnp.abs(v)))


def local_state(head, prompt, bias_ref, shift_ref, pieces):
    rows = shift_ref.shape[3]
    total = sum(ref[prompt, 0:rows, :].astype(F32) for ref in pieces)
    gates = sum(load_gates(ref[prompt, rows : rows + 32, :]) for ref in pieces)
    keys = total[:, 0:128].astype(BF16)
    values = total[:, 128:256].astype(BF16)
    length = gates.shape[1]
    shift = shift_ref[prompt, :, 0, :]
    row4 = lax.broadcasted_iota(jnp.int32, (4, length), 0)
    bias = jnp.where(row4 == 1, bias_ref[0, head], bias_ref[1, head])
    gates = gates[0:4, :]
    entry = gates + shift
    forget = log_sigmoid(gates + bias) + shift
    blocks = length // 128
    tall = jnp.concatenate([forget[:, 128 * b : 128 * b + 128] for b in range(blocks)], axis=0)
    r = lax.broadcasted_iota(jnp.int32, (128, 128), 0)
    c = lax.broadcasted_iota(jnp.int32, (128, 128), 1)
    climb = jnp.dot(tall, (r <= c).astype(F32), precision=lax.Precision.HIGHEST, preferred_element_type=F32)
    carry = jnp.zeros((4, 1), F32)
    parts = []
    for b in range(blocks):
        block = climb[4 * b : 4 * b + 4, :]
        parts.append(block + carry)
        carry = carry + block[:, 127:128]
    climb = jnp.concatenate(parts, axis=1)
    weight_fwd = carry[1:2] - climb[1:2] + entry[0:1]
    weight_bwd = climb[3:4] - forget[3:4] + entry[2:3]
    keys_t = jnp.transpose(keys.astype(F32))
    scale = HEAD ** -0.5
    memories, norms, tops, totals = [], [], [], []
    for weight, total in ((weight_fwd, carry[1:2]), (weight_bwd, carry[3:4])):
        top = jnp.max(weight, axis=1, keepdims=True)
        now = jnp.exp(weight - top)
        weighted = (keys_t * now).astype(BF16)
        memories.append(jnp.dot(weighted, values, preferred_element_type=F32) * scale)
        high = now.astype(BF16)
        low = (now - high.astype(F32)).astype(BF16)
        both = jnp.concatenate([high, low, jnp.zeros((6, length), BF16)], axis=0)
        norm = jnp.dot(both, keys, preferred_element_type=F32)
        norms.append((norm[0:1] + norm[1:2]) * scale)
        tops.append(jnp.broadcast_to(top, (1, 128)))
        totals.append(jnp.broadcast_to(total, (1, 128)))
    return memories, norms, totals, tops


def split_three(values):
    high = values.astype(BF16).astype(F32)
    rest = values - high
    middle = rest.astype(BF16).astype(F32)
    return high, middle, rest - middle


def small_tile(norms, totals, tops):
    norm_high = norms.astype(BF16).astype(F32)
    high, middle, low = split_three(jnp.concatenate([totals, tops], axis=0))
    lane = lax.broadcasted_iota(jnp.int32, high.shape, 1)
    parts = jnp.where(lane < 32, high, jnp.where(lane < 64, middle, low))
    return jnp.concatenate([norm_high, norms - norm_high, parts], axis=0).astype(BF16)


def state_kernel(bias_ref, shift_ref, a_ref, b_ref, c_ref, d_ref, out_ref):
    head = lax.axis_index("y") * 4 + lax.axis_index("x")
    memories, norms, totals, tops = [], [], [], []
    for p in range(2):
        found = local_state(head, p, bias_ref, shift_ref, (a_ref, b_ref, c_ref, d_ref))
        for have, more in zip((memories, norms, totals, tops), found):
            have.extend(more)
    tile = small_tile(*(jnp.concatenate(v, axis=0) for v in (norms, totals, tops)))
    for g in range(8):
        for i in range(4):
            out_ref[g, 16 * i : 16 * i + 16, :] = memories[i][16 * g : 16 * g + 16, :].astype(BF16)
        out_ref[g, 64:80, :] = tile


def merged(in_ref, count):
    tiles = [in_ref[g, 64:80, :].astype(F32) for g in range(count)]
    norms = [t[0:4] + t[4:8] for t in tiles]
    scalars = []
    for t in tiles:
        parts = t[8:16]
        whole = parts[:, 0:1] + parts[:, 32:33] + parts[:, 64:65]
        scalars.append(jnp.broadcast_to(whole, (8, 128)))
    totals = [s[0:4] for s in scalars]
    tops = [s[4:8] for s in scalars]
    row = lax.broadcasted_iota(jnp.int32, (4, 128), 0)
    before, after = [jnp.zeros((4, 128), F32)], [jnp.zeros((4, 128), F32)]
    for g in range(count - 1):
        before.append(before[-1] + totals[g])
        after.append(after[-1] + totals[count - 1 - g])
    whole = before[-1] + totals[-1]
    after = after[::-1]
    tops = [t + jnp.where(row % 2 == 0, after[g], before[g]) for g, t in enumerate(tops)]
    top = tops[0]
    for t in tops[1:]:
        top = jnp.maximum(top, t)
    return norms, tops, whole, top


def weighted_sums(in_ref, count, norms, tops, top):
    factors = [jnp.exp(t - top) for t in tops]
    norm = sum(f * n for f, n in zip(factors, norms))
    blocks = []
    for i in range(4):
        total = jnp.zeros((16, 128), F32)
        for g in range(count):
            total = total + in_ref[g, 16 * i : 16 * i + 16, :].astype(F32) * factors[g][i : i + 1]
        blocks.append(total)
    return norm, blocks


def group_merge_kernel(in_ref, out_ref):
    norms, tops, whole, top = merged(in_ref, 8)
    norm, blocks = weighted_sums(in_ref, 8, norms, tops, top)
    tile = small_tile(norm, whole, top)
    for g in range(4):
        for i in range(4):
            out_ref[g, 16 * i : 16 * i + 16, :] = blocks[i].astype(BF16)
        out_ref[g, 64:80, :] = tile


def last_merge_kernel(in_ref, out_ref, norm_ref, max_ref):
    norms, tops, whole, top = merged(in_ref, 4)
    top = jnp.maximum(whole, top)
    norm, blocks = weighted_sums(in_ref, 4, norms, tops, top)
    for g in range(8):
        for i in range(4):
            out_ref[g, 16 * i : 16 * i + 16, :] = blocks[i].astype(BF16)
    for i in range(4):
        norm_ref[i // 2, i % 2, :, :] = norm[i : i + 1]
        max_ref[i // 2, :, i % 2 : i % 2 + 1] = top[i : i + 1, 0:1]


def read_kernel(in_ref, norm_ref, query_ref, matrix_ref, read_ref):
    for g in range(8):
        for i in range(4):
            matrix_ref[i // 2, i % 2, 0, 16 * g : 16 * g + 16, :] = in_ref[g, 16 * i : 16 * i + 16, :]
    for p in range(2):
        query = query_ref[p]
        wide = query.astype(F32)
        total = jnp.zeros(wide.shape, F32)
        for j in range(2):
            i = 2 * p + j
            numerator = jnp.dot(query, matrix_ref[p, j, 0], preferred_element_type=F32)
            inner = jnp.sum(wide * norm_ref[p, j, :, :], axis=1, keepdims=True)
            total = total + numerator / jnp.maximum(jnp.abs(inner), 1.0)
        read_ref[p] = total.astype(BF16)


def program(tokens, w_key, w_value, w_gate, forget_bias, log_shift, new_query):
    prompts, length, width = tokens.shape
    depth = 4 * width
    near = {k: gather_from(tokens, k) for k in (1, 3)}
    far = [gather_from(near[k][p : p + 1], k) for p, k in enumerate((1, 3))]
    pieces = [tokens, near[1], *far, near[3]]
    packed_shapes = tuple(shape(depth, HEAD if k == 2 else 2 * HEAD) for k in range(4))
    weights = call(pack_weights_kernel, packed_shapes)(w_key, w_value)
    weights = [weights[0]] + [scatter_to(weights[k], k) for k in (1, 2, 3)]
    gate = w_gate.transpose(2, 1, 0)
    gate = jnp.concatenate([gate, gate], axis=1).reshape(128, 16, width).transpose(1, 0, 2)
    weights[2], gate = lax.optimization_barrier((weights[2], gate))
    swapped = lax.ppermute(weights[2], "zb", [(i, i ^ 1) for i in range(4)])
    weights = [(weights[0],), (weights[3],), (weights[2], swapped), (weights[1],)]
    gates = call(gates_kernel, shape(prompts, 128, length, dtype=F32))(*pieces, gate)
    partial = []
    for k in range(4):
        project = call(
            functools.partial(project_kernel, k),
            shape(prompts, length + 32, 2 * HEAD),
            flops=2 * prompts * length * depth * 256,
        )
        part = project(*pieces, *weights[k], gates)
        partial.append(scatter_to(part, k) if k else part)
    smem = pl.BlockSpec(memory_space=pltpu.SMEM)
    vmem = pl.BlockSpec(memory_space=pltpu.VMEM)
    packed = call(state_kernel, shape(8, 80, HEAD), in_specs=[smem] + [vmem] * 5)(forget_bias, log_shift, *partial)
    grouped = call(group_merge_kernel, shape(4, 80, HEAD))(exchange(packed, GROUP))
    slices, norm, top = call(
        last_merge_kernel, (shape(8, 64, HEAD), shape(2, 2, 1, HEAD, dtype=F32), shape(2, 1, 2, dtype=F32))
    )(exchange(grouped, "za"))
    matrix, read = call(read_kernel, (shape(2, 2, 1, HEAD, HEAD), shape(*new_query.shape)))(
        exchange(slices, GROUP), norm, new_query
    )
    return matrix, norm, top.transpose(0, 2, 1), read


def solution(mesh):
    finer = Mesh(mesh.devices.reshape(4, 4, 2, 4, 4), ("za", "zb", "c", "y", "x"))
    tp = ("y", "x")
    in_specs = (
        P(None, SP, tp),
        P(None, tp),
        P(None, tp),
        P(),
        P(),
        P(None, None, tp, SP),
        P(None, SP, tp),
    )
    out_specs = (
        P(None, None, tp, None, None),
        P(None, None, tp, None),
        P(None, None, tp),
        P(None, SP, tp),
    )
    return jax.shard_map(program, mesh=finer, in_specs=in_specs, out_specs=out_specs, check_vma=False)
```
